32 devices in a mesh: sp: 8 (over z, y), tp: 4 (over x, core).
Axes of the slice: x: 2, y: 2, z: 4, core: 2. Of those that a mesh axis runs over, the one named last changes fastest.
Arguments:
- out_cotangent: bfloat16 [1024, 2048], P('sp', 'tp'), may hold values from -6 to 6
- expert_input: bfloat16 [1024, 2048], P('sp', 'tp'), may hold values from -6 to 6
- routes: int32 [1024, 2], P('sp'), may hold values from 0 to 7, as said below
- route_weights: float32 [1024, 2], P('sp'), may hold values from 0.2 to 1
- gate_proj: bfloat16 [8, 2048, 3584], P('sp', None, 'tp'), may hold values from -0.125 to 0.125
- up_proj: bfloat16 [8, 2048, 3584], P('sp', None, 'tp'), may hold values from -0.125 to 0.125
- down_proj: bfloat16 [8, 3584, 2048], P('sp', 'tp'), may hold values from -0.09375 to 0.09375
- conv_out: bfloat16 [1024, 2048], P('sp', 'tp'), may hold values from -27 to 27
- conv_mean: float32 [1024], P('sp'), may hold values from -3 to 3
- conv_rstd: float32 [1024], P('sp'), may hold values from 0.25 to 1
- norm_gain: float32 [2048], P('tp'), may hold values from 0.1 to 1.9
- taps: float32 [31, 2048], P(None, 'tp'), may hold values from -1 to 1
- out_proj: bfloat16 [2048, 2048], P(None, 'tp'), may hold values from -0.125 to 0.125
Outputs:
- gate_grad: bfloat16 [8, 2048, 3584], P('sp', None, 'tp')
- up_grad: bfloat16 [8, 2048, 3584], P('sp', None, 'tp')
- down_grad: bfloat16 [8, 3584, 2048], P('sp', 'tp')
- proj_grad: float32 [2048, 2048], P('sp', 'tp')
- stream_grad: bfloat16 [1024, 2048], P('sp', 'tp')
- conv_in_grad: bfloat16 [1024, 2048], P('sp', 'tp')
The draws below stay inside these ranges and needn't reach their ends.
Inputs may be any that keep to these rules, and one draw needn't show every extreme that they name: `routes`: each row names 2 different experts. In each aligned block of 128 rows (the rows of one device) no expert is named by more than 48 rows, and one expert, the same in every block, is named by exactly 48 rows of every block.
All inputs are finite; a program needn't handle non-finite values.
Results may differ from the reference program's by a relative error of at most 0.02.
Values may be sent and summed in bfloat16 or wider, within the bound.
No kernel may reach another device: no remote copies, remote signals or barrier semaphores. Data moves between devices by JAX's collectives and lax.ppermute only.
A program may use at most 128 MiB of HBM per device.

```python
import math
import jax
import jax.numpy as jnp
from jax import lax

D = 2048
FF = 3584
TOP = 2
TAPS = 31
TOK_DEV = 128
EXPERTS = 8
CAP = 48
TOKENS = 1024
HID_BLOCKS = 4


def draw_routes(key, part):
    blocks = TOKENS // TOK_DEV
    hot_key, rest_key = jax.random.split(jax.random.fold_in(key, 11))
    hottest = jax.random.randint(hot_key, (), 0, EXPERTS).astype(jnp.int32)
    block_keys = jax.random.split(rest_key, blocks)
    spare = 2 * TOK_DEV - CAP
    base_count = spare // (EXPERTS - 1)
    extra_count = spare % (EXPERTS - 1)
    shift_reach = min(base_count, CAP - base_count - 1)
    pair_count = (EXPERTS - 1) // 2

    def one_block(block_key):
        perm_key, shift_key, row_key, side_key = jax.random.split(block_key, 4)
        others = jax.random.permutation(perm_key, EXPERTS - 1).astype(jnp.int32)
        others = others + (others >= hottest).astype(jnp.int32)
        expert_order = jnp.concatenate([hottest[None], others])
        counts = base_count + (jnp.arange(EXPERTS - 1) < extra_count).astype(jnp.int32)
        moves = jax.random.randint(shift_key, (pair_count,), 0, shift_reach + 1).astype(jnp.int32)
        change = jnp.concatenate([jnp.stack([moves, -moves], axis=1).reshape(-1), jnp.zeros((EXPERTS - 1 - 2 * pair_count,), jnp.int32)])
        counts = jnp.concatenate([jnp.full((1,), CAP, jnp.int32), counts + change])
        run_ends = jnp.cumsum(counts)
        position = jnp.arange(2 * TOK_DEV, dtype=jnp.int32)
        run_index = jnp.sum((position[:, None] >= run_ends[None, :]).astype(jnp.int32), axis=1)
        labels = expert_order[run_index]
        first_half = labels[:TOK_DEV]
        second_half = labels[TOK_DEV:]
        row_order = jax.random.permutation(row_key, TOK_DEV)
        flipped = jax.random.randint(side_key, (TOK_DEV,), 0, 2)
        left_col = jnp.where(flipped == 1, second_half, first_half)[row_order]
        right_col = jnp.where(flipped == 1, first_half, second_half)[row_order]
        return jnp.stack([left_col, right_col], axis=1)
    return jax.vmap(one_block)(block_keys).reshape(TOKENS, TOP).astype(jnp.int32)


def draw_conv_out(key, part):
    noise_key, rough_key = jax.random.split(jax.random.fold_in(key, 23))
    channel = jnp.arange(D, dtype=jnp.float32)
    rising = jnp.exp(jnp.log(3.0) * channel / (D - 1))
    rough = jax.random.uniform(rough_key, (D,), jnp.float32, 0.6, 1.5)
    values = jnp.clip(jax.random.normal(noise_key, (TOKENS, D), jnp.float32), -6.0, 6.0)
    return (values * rising[None, :] * rough[None, :]).astype(jnp.bfloat16)


def spiked(result, stream_key, source, target, shards_of, factor):
    owner, partner = [(jnp.arange(result.shape[dim]) // (result.shape[dim] // shards_of)).reshape([-1 if axis == dim else 1 for axis in range(result.ndim)]) for dim in (source, target)]
    chosen = jax.random.permutation(stream_key, shards_of)[partner]
    strong = (owner == chosen) | (owner == (partner + shards_of // 2) % shards_of)
    return jnp.where(strong, factor * result, result)


def levels(own_key, extent, pieces, smallest, largest):
    loudness, own = 1.0, jax.random.fold_in(own_key, 6)
    for axis_at, blocks in pieces:
        draws = jnp.exp(jax.random.uniform(jax.random.fold_in(own, axis_at), (blocks,), jnp.float32, smallest / len(pieces), largest / len(pieces)))
        loudness = loudness * jnp.repeat(draws, extent[axis_at] // blocks).reshape([-1 if axis == axis_at else 1 for axis in range(len(extent))])
    return loudness


def scatter_about(key, dims, deviation, bound, shards=(), kind=jnp.bfloat16):
    level = levels(key, dims, shards, -0.22, 0.18) if shards else 1.0
    drawn = jax.random.normal(key, dims, jnp.float32) * deviation * level
    return jnp.minimum(jnp.maximum(drawn, -bound), bound).astype(kind)


def noise_with(rng, dims, width, bound, cuts, heavy, kind=jnp.bfloat16):
    values = width * jax.random.normal(rng, dims, jnp.float32)
    if cuts:
        values = values * levels(rng, dims, cuts, -0.22, 0.18)
    return jnp.clip(spiked(values, jax.random.fold_in(rng, 3), *heavy), -bound, bound).astype(kind)


def setup_inputs(seed: int = 0) -> dict:
    splits = jax.random.split(jax.random.key(seed), 14)
    return {
        "out_cotangent": noise_with(splits[0], (TOKENS, D), 1.0, 6.0, ((0, 8), (1, 4)), (0, 1, 8, 2.0)),
        "expert_input": scatter_about(splits[1], (TOKENS, D), 1.0, 6.0, ((0, 8), (1, 4))),
        "routes": draw_routes(jax.random.fold_in(splits[13], 71), 0),
        "route_weights": jnp.clip(0.2 + 0.8 * jax.random.uniform(splits[3], (TOKENS, TOP), jnp.float32) ** levels(splits[3], (TOKENS, TOP), ((0, 8),), -0.2, 0.2), 0.2, 1.0),
        "gate_proj": scatter_about(splits[4], (EXPERTS, D, FF), D ** -0.5, 0.125, ((0, 8), (2, 4))),
        "up_proj": scatter_about(splits[5], (EXPERTS, D, FF), D ** -0.5, 0.125, ((0, 8), (2, 4))),
        "down_proj": scatter_about(splits[6], (EXPERTS, FF, D), FF ** -0.5, 0.09375, ((0, 8), (1, 4))),
        "conv_out": draw_conv_out(jax.random.fold_in(splits[13], 71), 0),
        "conv_mean": scatter_about(splits[8], (TOKENS,), 0.5, 3.0, ((0, 8),), jnp.float32),
        "conv_rstd": jnp.clip(jnp.exp(math.log(1.0) - 1.3862944 * jax.random.uniform(splits[9], (TOKENS,), jnp.float32) ** levels(splits[9], (TOKENS,), ((0, 8),), -0.2, 0.2)), 0.25, 1.0),
        "norm_gain": jnp.clip(1.0 + 0.18 * jax.random.normal(splits[10], (D,), jnp.float32), 0.1, 1.9),
        "taps": scatter_about(splits[11], (TAPS, D), TAPS ** -0.5, 1.0, ((1, 4),), jnp.float32),
        "out_proj": scatter_about(splits[12], (D, D), D ** -0.5, 0.125, ((1, 4),)),
    }


OUTER_DIMS = (((0,), (0,)), ((), ()))
INNER_DIMS = (((1,), (1,)), ((), ()))


def reference(out_cotangent, expert_input, routes, route_weights, gate_proj, up_proj, down_proj, conv_out, conv_mean, conv_rstd, norm_gain, taps, out_proj):
    assigned = routes.reshape(-1).astype(jnp.int32)
    pair_weights = route_weights.reshape(-1)
    limit = CAP * EXPERTS
    outside = TOKENS * TOP
    block_width = FF // HID_BLOCKS

    def one_expert(expert_id):
        picked = jnp.nonzero(assigned == expert_id, size=limit, fill_value=outside)[0].astype(jnp.int32)
        usable = picked < outside
        safe_pair = jnp.where(usable, picked, 0)
        token_index = safe_pair // TOP
        rows = jnp.where(usable[:, None], expert_input[token_index], jnp.zeros((), jnp.bfloat16))
        weight = jnp.where(usable, pair_weights[safe_pair], 0.0)
        routed_cot = (weight[:, None] * out_cotangent[token_index].astype(jnp.float32)).astype(jnp.bfloat16)
        gate_local = gate_proj[expert_id]
        up_local = up_proj[expert_id]
        down_local = down_proj[expert_id]
        gate_pre = jnp.dot(rows, gate_local, preferred_element_type=jnp.float32)
        up_pre = jnp.dot(rows, up_local, preferred_element_type=jnp.float32)
        gate_sigmoid = jax.nn.sigmoid(gate_pre)
        activation = (gate_pre * gate_sigmoid * up_pre).astype(jnp.bfloat16)
        act_grad = lax.dot_general(routed_cot, down_local, INNER_DIMS, preferred_element_type=jnp.float32)
        gate_back = (act_grad * up_pre * gate_sigmoid * (1.0 + gate_pre * (1.0 - gate_sigmoid))).astype(jnp.bfloat16)
        up_back = (act_grad * gate_pre * gate_sigmoid).astype(jnp.bfloat16)
        down_part = lax.dot_general(activation, routed_cot, OUTER_DIMS, preferred_element_type=jnp.float32).astype(jnp.bfloat16)
        gate_part = lax.dot_general(rows, gate_back, OUTER_DIMS, preferred_element_type=jnp.float32).astype(jnp.bfloat16)
        up_part = lax.dot_general(rows, up_back, OUTER_DIMS, preferred_element_type=jnp.float32).astype(jnp.bfloat16)
        block_parts = jnp.einsum('lbu,dbu->lbd', gate_back.astype(jnp.float32).reshape(limit, HID_BLOCKS, block_width), gate_local.astype(jnp.float32).reshape(D, HID_BLOCKS, block_width))
        block_parts = block_parts + jnp.einsum('lbu,dbu->lbd', up_back.astype(jnp.float32).reshape(limit, HID_BLOCKS, block_width), up_local.astype(jnp.float32).reshape(D, HID_BLOCKS, block_width))
        block_parts = block_parts.astype(jnp.bfloat16)
        routed_grad = jnp.sum(block_parts.astype(jnp.float32), axis=1).astype(jnp.bfloat16)
        return gate_part, up_part, down_part, routed_grad, picked

    gate_grad, up_grad, down_grad, routed_grad, picked = lax.map(one_expert, jnp.arange(EXPERTS, dtype=jnp.int32))
    placed = jnp.zeros((outside, D), jnp.bfloat16).at[picked.reshape(-1)].set(routed_grad.reshape(-1, D), mode="drop")
    routed_sum = jnp.sum(placed.reshape(TOKENS, TOP, D).astype(jnp.float32), axis=1)
    stream_grad = (out_cotangent.astype(jnp.float32) + routed_sum).astype(jnp.bfloat16)

    normed = (conv_out.astype(jnp.float32) - conv_mean[:, None]) * conv_rstd[:, None]
    scaled = normed * norm_gain[None, :]
    scaled_sigmoid = jax.nn.sigmoid(scaled)
    swished = (scaled * scaled_sigmoid).astype(jnp.bfloat16)
    proj_grad = lax.dot_general(stream_grad, swished, OUTER_DIMS, preferred_element_type=jnp.float32)
    swished_grad = jnp.dot(stream_grad, out_proj, preferred_element_type=jnp.float32)
    scaled_grad = swished_grad * scaled_sigmoid * (1.0 + scaled * (1.0 - scaled_sigmoid)) * norm_gain[None, :]
    first_mean = jnp.mean(scaled_grad, axis=1, keepdims=True)
    second_mean = jnp.mean(scaled_grad * normed, axis=1, keepdims=True)
    conv_grad = conv_rstd[:, None] * (scaled_grad - first_mean - normed * second_mean)
    padded = jnp.concatenate([conv_grad, jnp.zeros((TAPS - 1, D), jnp.float32)], axis=0)
    conv_sum = jnp.zeros((TOKENS, D), jnp.float32)
    for offset in range(TAPS):
        conv_sum = conv_sum + taps[offset][None, :] * padded[offset:offset + TOKENS]
    return gate_grad, up_grad, down_grad, proj_grad, stream_grad, conv_sum.astype(jnp.bfloat16)
```

```python
import jax
import jax.numpy as jnp
from jax import lax
from jax.experimental import pallas as pl
from jax.experimental.pallas import tpu as pltpu
from jax.sharding import PartitionSpec as P

OUTER_DIMS = (((0,), (0,)), ((), ()))
INNER_DIMS = (((1,), (1,)), ((), ()))


def swapped(value, axis, mask):
    count = lax.axis_size(axis)
    return lax.ppermute(value, axis, [(source, source ^ mask) for source in range(count)])


def passed_back(value, axis):
    count = lax.axis_size(axis)
    return lax.ppermute(value, axis, [(source, source - 1) for source in range(1, count)])


def exchanged(chunks, axis):
    return [chunks[0]] + [swapped(chunk, axis, k) for k, chunk in enumerate(chunks) if k]


def gathered(value, axis):
    count = lax.axis_size(axis)
    here = lax.axis_index(axis)
    step = 1
    bits = []
    while step < count:
        bits.append(step)
        step *= 2
    found = {0: value}
    for bit in reversed(bits):
        for offset in list(found):
            found[offset | bit] = swapped(found[offset], axis, bit)
    parts = [found[k] for k in range(count)]
    for bit in bits:
        odd = (here & bit) != 0
        parts = [jnp.where(odd, parts[k ^ bit], parts[k]) for k in range(count)]
    return jnp.concatenate(parts, axis=1)


def dispatch(routes, weights, tokens, cotangent, experts, capacity):
    tok_rows, width = tokens.shape
    slots = experts * capacity

    def kernel(here, routes, weights, tokens, cotangent, rows, cots, places):
        rel = routes[...] ^ here[0]
        rel_a, rel_b = rel[0:1], rel[1:2]
        ids = lax.broadcasted_iota(jnp.int32, (experts, tok_rows), 0)
        hit_a, hit_b = ids == rel_a, ids == rel_b
        hits = jnp.where(hit_a | hit_b, 1.0, 0.0).astype(jnp.bfloat16)
        before = lax.broadcasted_iota(jnp.int32, (tok_rows, tok_rows), 0)
        after = lax.broadcasted_iota(jnp.int32, (tok_rows, tok_rows), 1)
        tri = jnp.where(before < after, 1.0, 0.0).astype(jnp.bfloat16)
        rank = jnp.dot(hits, tri, preferred_element_type=jnp.float32)
        rank_a = jnp.sum(jnp.where(hit_a, rank, 0.0), axis=0, keepdims=True).astype(jnp.int32)
        rank_b = jnp.sum(jnp.where(hit_b, rank, 0.0), axis=0, keepdims=True).astype(jnp.int32)
        slot = lax.broadcasted_iota(jnp.int32, (slots, tok_rows), 0)
        at_a = slot == rel_a * capacity + rank_a
        at_b = slot == rel_b * capacity + rank_b
        place = jnp.where(at_a | at_b, 1.0, 0.0).astype(jnp.bfloat16)
        scale = jnp.sum(
            jnp.where(at_a, weights[0:1], 0.0) + jnp.where(at_b, weights[1:2], 0.0),
            axis=1,
            keepdims=True,
        )
        places[...] = place
        rows[...] = jnp.dot(place, tokens[...], preferred_element_type=jnp.float32).astype(
            jnp.bfloat16
        )
        picked = jnp.dot(place, cotangent[...], preferred_element_type=jnp.float32)
        cots[...] = (scale * picked).astype(jnp.bfloat16)

    here = lax.axis_index("sp").astype(jnp.int32).reshape(1)
    whole = pl.BlockSpec(memory_space=pltpu.VMEM)
    return pl.pallas_call(
        kernel,
        out_shape=(
            jax.ShapeDtypeStruct((slots, width), jnp.bfloat16),
            jax.ShapeDtypeStruct((slots, width), jnp.bfloat16),
            jax.ShapeDtypeStruct((slots, tok_rows), jnp.bfloat16),
        ),
        in_specs=[pl.BlockSpec(memory_space=pltpu.SMEM)] + [whole] * 4,
        out_specs=(whole, whole, whole),
        name="dispatch",
    )(here, routes.T, weights.T, tokens, cotangent)


def body(
    out_cotangent,
    expert_input,
    routes,
    route_weights,
    gate_proj,
    up_proj,
    down_proj,
    conv_out,
    conv_mean,
    conv_rstd,
    norm_gain,
    taps,
    out_proj,
):
    tok_rows, local_width = out_cotangent.shape
    experts = lax.axis_size("sp")
    width_parts = lax.axis_size("tp")
    full_width = local_width * width_parts
    capacity = 3 * tok_rows // experts
    sp_at = lax.axis_index("sp")
    tp_at = lax.axis_index("tp")
    rows_out, cots_out, places = dispatch(
        routes, route_weights, expert_input, out_cotangent, experts, capacity
    )

    def chunked(value):
        return [value[k * capacity : (k + 1) * capacity] for k in range(experts)]

    rows_mid = jnp.concatenate(exchanged(chunked(rows_out), "sp"), axis=0)
    cots_mid = jnp.concatenate(exchanged(chunked(cots_out), "sp"), axis=0)
    rows_in = gathered(rows_mid, "tp")
    cot_in = gathered(cots_mid, "tp")
    gate_local = gate_proj[0]
    up_local = up_proj[0]
    down_local = down_proj[0]

    conv_ready, _ = lax.optimization_barrier((conv_out, cots_mid))
    normed = (conv_ready.astype(jnp.float32) - conv_mean[:, None]) * conv_rstd[:, None]
    scaled = normed * norm_gain[None, :]
    scaled_sigmoid = jax.nn.sigmoid(scaled)
    swished = (scaled * scaled_sigmoid).astype(jnp.bfloat16)
    swished_all = jnp.concatenate(exchanged([swished] * experts, "sp"), axis=0)

    gate_pre = jnp.dot(rows_in, gate_local, preferred_element_type=jnp.float32)
    up_pre = jnp.dot(rows_in, up_local, preferred_element_type=jnp.float32)
    gate_sigmoid = jax.nn.sigmoid(gate_pre)
    activation = (gate_pre * gate_sigmoid * up_pre).astype(jnp.bfloat16)
    act_grad = lax.dot_general(cot_in, down_local, INNER_DIMS, preferred_element_type=jnp.float32)
    gate_back = (act_grad * up_pre * gate_sigmoid * (1.0 + gate_pre * (1.0 - gate_sigmoid))).astype(
        jnp.bfloat16
    )
    up_back = (act_grad * gate_pre * gate_sigmoid).astype(jnp.bfloat16)

    def partial_block(mask):
        start = (tp_at ^ mask) * local_width
        gate_rows = lax.dynamic_slice_in_dim(gate_local, start, local_width, axis=0)
        up_rows = lax.dynamic_slice_in_dim(up_local, start, local_width, axis=0)
        return lax.dot_general(
            gate_back, gate_rows, INNER_DIMS, preferred_element_type=jnp.float32
        ) + lax.dot_general(up_back, up_rows, INNER_DIMS, preferred_element_type=jnp.float32)

    def summed_over(offsets, bit):
        if bit == 0:
            return partial_block(offsets)
        lower = bit // 2
        away = summed_over(offsets | bit, lower).astype(jnp.bfloat16)
        away = swapped(away, "tp", bit)
        return summed_over(offsets, lower) + away.astype(jnp.float32)

    summed = summed_over(0, width_parts // 2).astype(jnp.bfloat16)
    routed = jnp.concatenate(exchanged(chunked(summed), "sp"), axis=0)
    down_grad = lax.dot_general(
        activation, cot_in, OUTER_DIMS, preferred_element_type=jnp.float32
    ).astype(jnp.bfloat16)[None]
    gate_grad = lax.dot_general(
        rows_in, gate_back, OUTER_DIMS, preferred_element_type=jnp.float32
    ).astype(jnp.bfloat16)[None]
    up_grad = lax.dot_general(
        rows_in, up_back, OUTER_DIMS, preferred_element_type=jnp.float32
    ).astype(jnp.bfloat16)[None]
    routed_sum = lax.dot_general(places, routed, OUTER_DIMS, preferred_element_type=jnp.float32)
    stream = (out_cotangent.astype(jnp.float32) + routed_sum).astype(jnp.bfloat16)
    stream_whole = gathered(stream, "tp")

    feature_rows = full_width // experts
    feature_chunks = [
        lax.dynamic_slice_in_dim(stream_whole, (sp_at ^ k) * feature_rows, feature_rows, axis=1)
        for k in range(experts)
    ]
    stream_all = jnp.concatenate(exchanged(feature_chunks, "sp"), axis=0)
    proj_grad = lax.dot_general(
        stream_all, swished_all, OUTER_DIMS, preferred_element_type=jnp.float32
    )

    swished_grad = jnp.dot(stream_whole, out_proj, preferred_element_type=jnp.float32)
    scaled_grad = (
        swished_grad * scaled_sigmoid * (1.0 + scaled * (1.0 - scaled_sigmoid)) * norm_gain[None, :]
    )
    stat_parts = jnp.stack([jnp.sum(scaled_grad, axis=1), jnp.sum(scaled_grad * normed, axis=1)])
    stat_sums = stat_parts
    for mask in range(1, width_parts):
        stat_sums = stat_sums + swapped(stat_parts, "tp", mask)
    first_mean = stat_sums[0][:, None] / full_width
    second_mean = stat_sums[1][:, None] / full_width
    conv_grad = conv_rstd[:, None] * (scaled_grad - first_mean - normed * second_mean)
    halo_rows = taps.shape[0] - 1
    following = passed_back(conv_grad[:halo_rows].astype(jnp.bfloat16), "sp").astype(jnp.float32)
    extended = jnp.concatenate([conv_grad, following], axis=0)
    conv_sum = jnp.zeros((tok_rows, local_width), jnp.float32)
    for offset in range(halo_rows + 1):
        conv_sum = conv_sum + taps[offset][None, :] * extended[offset : offset + tok_rows]
    return (gate_grad, up_grad, down_grad, proj_grad, stream, conv_sum.astype(jnp.bfloat16))


def solution(mesh):
    in_specs = (
        P("sp", "tp"),
        P("sp", "tp"),
        P("sp", None),
        P("sp", None),
        P("sp", None, "tp"),
        P("sp", None, "tp"),
        P("sp", "tp", None),
        P("sp", "tp"),
        P("sp"),
        P("sp"),
        P("tp"),
        P(None, "tp"),
        P(None, "tp"),
    )
    out_specs = (
        P("sp", None, "tp"),
        P("sp", None, "tp"),
        P("sp", "tp", None),
        P("sp", "tp"),
        P("sp", "tp"),
        P("sp", "tp"),
    )
    return jax.shard_map(body, mesh=mesh, in_specs=in_specs, out_specs=out_specs, check_vma=False)
```

```python
import jax
import jax.numpy as jnp
from jax import lax
from jax.experimental import pallas as pl
from jax.experimental.pallas import tpu as pltpu
from jax.sharding import PartitionSpec as P

OUTER_DIMS = (((0,), (0,)), ((), ()))
INNER_DIMS = (((1,), (1,)), ((), ()))


def swapped(value, axis, mask):
    count = lax.axis_size(axis)
    return lax.ppermute(value, axis, [(source, source ^ mask) for source in range(count)])


def passed_back(value, axis):
    count = lax.axis_size(axis)
    return lax.ppermute(value, axis, [(source, source - 1) for source in range(1, count)])


def exchanged(chunks, axis):
    return [chunks[0]] + [swapped(chunk, axis, k) for k, chunk in enumerate(chunks) if k]


def bits_of(axis):
    count = lax.axis_size(axis)
    return [1 << n for n in range(count.bit_length() - 1)]


def stacked_gather(value, axis):
    for bit in reversed(bits_of(axis)):
        value = jnp.concatenate([value, swapped(value, axis, bit)], axis=0)
    return value


def stacked_exchange(value, axis):
    for bit in reversed(bits_of(axis)):
        half = value.shape[1] // 2
        value = jnp.concatenate([value[:, :half], swapped(value[:, half:], axis, bit)], axis=0)
    return value


def gathered(value, axis):
    count = lax.axis_size(axis)
    here = lax.axis_index(axis)
    bits = bits_of(axis)
    found = {0: value}
    for bit in reversed(bits):
        for offset in list(found):
            found[offset | bit] = swapped(found[offset], axis, bit)
    parts = [found[k] for k in range(count)]
    for bit in bits:
        odd = (here & bit) != 0
        parts = [jnp.where(odd, parts[k ^ bit], parts[k]) for k in range(count)]
    return jnp.concatenate(parts, axis=1)


def dispatch(routes, weights, tokens, cotangent, experts, capacity):
    tok_rows, width = tokens.shape
    slots = experts * capacity

    def kernel(here, routes, weights, tokens, cotangent, payload, places):
        rel = routes[...] ^ here[0]
        rel_a, rel_b = rel[0:1], rel[1:2]
        ids = lax.broadcasted_iota(jnp.int32, (experts, tok_rows), 0)
        hit_a, hit_b = ids == rel_a, ids == rel_b
        hits = jnp.where(hit_a | hit_b, 1.0, 0.0).astype(jnp.bfloat16)
        before = lax.broadcasted_iota(jnp.int32, (tok_rows, tok_rows), 0)
        after = lax.broadcasted_iota(jnp.int32, (tok_rows, tok_rows), 1)
        tri = jnp.where(before < after, 1.0, 0.0).astype(jnp.bfloat16)
        rank = jnp.dot(hits, tri, preferred_element_type=jnp.float32)
        rank_a = jnp.sum(jnp.where(hit_a, rank, 0.0), axis=0, keepdims=True).astype(jnp.int32)
        rank_b = jnp.sum(jnp.where(hit_b, rank, 0.0), axis=0, keepdims=True).astype(jnp.int32)
        slot = lax.broadcasted_iota(jnp.int32, (slots, tok_rows), 0)
        at_a = slot == rel_a * capacity + rank_a
        at_b = slot == rel_b * capacity + rank_b
        place = jnp.where(at_a | at_b, 1.0, 0.0).astype(jnp.bfloat16)
        scale = jnp.sum(
            jnp.where(at_a, weights[0:1], 0.0) + jnp.where(at_b, weights[1:2], 0.0),
            axis=1,
            keepdims=True,
        )
        places[...] = place
        payload[:, :width] = jnp.dot(place, tokens[...], preferred_element_type=jnp.float32).astype(
            jnp.bfloat16
        )
        picked = jnp.dot(place, cotangent[...], preferred_element_type=jnp.float32)
        payload[:, width:] = (scale * picked).astype(jnp.bfloat16)

    here = lax.axis_index("sp").astype(jnp.int32).reshape(1)
    whole = pl.BlockSpec(memory_space=pltpu.VMEM)
    return pl.pallas_call(
        kernel,
        out_shape=(
            jax.ShapeDtypeStruct((slots, 2 * width), jnp.bfloat16),
            jax.ShapeDtypeStruct((slots, tok_rows), jnp.bfloat16),
        ),
        in_specs=[pl.BlockSpec(memory_space=pltpu.SMEM)] + [whole] * 4,
        out_specs=(whole, whole),
        name="dispatch",
    )(here, routes.T, weights.T, tokens, cotangent)


def body(
    out_cotangent,
    expert_input,
    routes,
    route_weights,
    gate_proj,
    up_proj,
    down_proj,
    conv_out,
    conv_mean,
    conv_rstd,
    norm_gain,
    taps,
    out_proj,
):
    tok_rows, local_width = out_cotangent.shape
    experts = lax.axis_size("sp")
    width_parts = lax.axis_size("tp")
    full_width = local_width * width_parts
    capacity = 3 * tok_rows // experts
    sp_at = lax.axis_index("sp")
    tp_at = lax.axis_index("tp")
    payload, places = dispatch(
        routes, route_weights, expert_input, out_cotangent, experts, capacity
    )

    def chunked(value):
        return [value[k * capacity : (k + 1) * capacity] for k in range(experts)]

    arrived = exchanged(chunked(payload), "sp")
    rows_mid = jnp.concatenate([chunk[:, :local_width] for chunk in arrived], axis=0)
    cots_mid = jnp.concatenate([chunk[:, local_width:] for chunk in arrived], axis=0)
    rows_in = gathered(rows_mid, "tp")
    cot_in = gathered(cots_mid, "tp")
    gate_local = gate_proj[0]
    up_local = up_proj[0]
    down_local = down_proj[0]

    conv_ready, _ = lax.optimization_barrier((conv_out, cots_mid))
    normed = (conv_ready.astype(jnp.float32) - conv_mean[:, None]) * conv_rstd[:, None]
    scaled = normed * norm_gain[None, :]
    scaled_sigmoid = jax.nn.sigmoid(scaled)
    swished = (scaled * scaled_sigmoid).astype(jnp.bfloat16)
    swished_all = stacked_gather(swished, "sp")

    gate_pre = jnp.dot(rows_in, gate_local, preferred_element_type=jnp.float32)
    up_pre = jnp.dot(rows_in, up_local, preferred_element_type=jnp.float32)
    gate_sigmoid = jax.nn.sigmoid(gate_pre)
    activation = (gate_pre * gate_sigmoid * up_pre).astype(jnp.bfloat16)
    act_grad = lax.dot_general(cot_in, down_local, INNER_DIMS, preferred_element_type=jnp.float32)
    gate_back = (act_grad * up_pre * gate_sigmoid * (1.0 + gate_pre * (1.0 - gate_sigmoid))).astype(
        jnp.bfloat16
    )
    up_back = (act_grad * gate_pre * gate_sigmoid).astype(jnp.bfloat16)

    down_grad = lax.dot_general(
        activation, cot_in, OUTER_DIMS, preferred_element_type=jnp.float32
    ).astype(jnp.bfloat16)[None]
    gate_grad = lax.dot_general(
        rows_in, gate_back, OUTER_DIMS, preferred_element_type=jnp.float32
    ).astype(jnp.bfloat16)[None]
    up_grad = lax.dot_general(
        rows_in, up_back, OUTER_DIMS, preferred_element_type=jnp.float32
    ).astype(jnp.bfloat16)[None]
    def partial_block(mask):
        start = (tp_at ^ mask) * local_width
        gate_rows = lax.dynamic_slice_in_dim(gate_local, start, local_width, axis=0)
        up_rows = lax.dynamic_slice_in_dim(up_local, start, local_width, axis=0)
        return lax.dot_general(
            gate_back, gate_rows, INNER_DIMS, preferred_element_type=jnp.float32
        ) + lax.dot_general(up_back, up_rows, INNER_DIMS, preferred_element_type=jnp.float32)

    covers = [down_grad, gate_grad]

    def summed_over(offsets, bit):
        if bit == 0:
            return partial_block(offsets)
        lower = bit // 2
        away = summed_over(offsets | bit, lower).astype(jnp.bfloat16)
        away = swapped(away, "tp", bit)
        if bit == width_parts // 2:
            away, covers[0], covers[1] = lax.optimization_barrier((away, covers[0], covers[1]))
        return summed_over(offsets, lower) + away.astype(jnp.float32)

    summed = summed_over(0, width_parts // 2).astype(jnp.bfloat16)
    down_grad, gate_grad = covers
    routed = jnp.concatenate(exchanged(chunked(summed), "sp"), axis=0)
    routed_sum = lax.dot_general(places, routed, OUTER_DIMS, preferred_element_type=jnp.float32)
    stream = (out_cotangent.astype(jnp.float32) + routed_sum).astype(jnp.bfloat16)
    stream_whole = gathered(stream, "tp")

    feature_rows = full_width // experts
    feature_chunks = [
        lax.dynamic_slice_in_dim(stream_whole, (sp_at ^ k) * feature_rows, feature_rows, axis=1)
        for k in range(experts)
    ]
    stream_all = stacked_exchange(jnp.concatenate(feature_chunks, axis=1), "sp")
    proj_grad = lax.dot_general(
        stream_all, swished_all, OUTER_DIMS, preferred_element_type=jnp.float32
    )

    swished_grad = jnp.dot(stream_whole, out_proj, preferred_element_type=jnp.float32)
    scaled_grad = (
        swished_grad * scaled_sigmoid * (1.0 + scaled * (1.0 - scaled_sigmoid)) * norm_gain[None, :]
    )
    stat_parts = jnp.stack([jnp.sum(scaled_grad, axis=1), jnp.sum(scaled_grad * normed, axis=1)])
    stat_sums = stat_parts
    for mask in range(1, width_parts):
        stat_sums = stat_sums + swapped(stat_parts, "tp", mask)
    first_mean = stat_sums[0][:, None] / full_width
    second_mean = stat_sums[1][:, None] / full_width
    conv_grad = conv_rstd[:, None] * (scaled_grad - first_mean - normed * second_mean)
    halo_rows = taps.shape[0] - 1
    following = passed_back(conv_grad[:halo_rows].astype(jnp.bfloat16), "sp").astype(jnp.float32)
    extended = jnp.concatenate([conv_grad, following], axis=0)
    conv_sum = jnp.zeros((tok_rows, local_width), jnp.float32)
    for offset in range(halo_rows + 1):
        conv_sum = conv_sum + taps[offset][None, :] * extended[offset : offset + tok_rows]
    return (gate_grad, up_grad, down_grad, proj_grad, stream, conv_sum.astype(jnp.bfloat16))


def solution(mesh):
    in_specs = (
        P("sp", "tp"),
        P("sp", "tp"),
        P("sp", None),
        P("sp", None),
        P("sp", None, "tp"),
        P("sp", None, "tp"),
        P("sp", "tp", None),
        P("sp", "tp"),
        P("sp"),
        P("sp"),
        P("tp"),
        P(None, "tp"),
        P(None, "tp"),
    )
    out_specs = (
        P("sp", None, "tp"),
        P("sp", None, "tp"),
        P("sp", "tp", None),
        P("sp", "tp"),
        P("sp", "tp"),
        P("sp", "tp"),
    )
    return jax.shard_map(body, mesh=mesh, in_specs=in_specs, out_specs=out_specs, check_vma=False)
```

```python
import jax
import jax.numpy as jnp
from jax import lax
from jax.experimental import pallas as pl
from jax.experimental.pallas import tpu as pltpu
from jax.sharding import PartitionSpec as P

OUTER_DIMS = (((0,), (0,)), ((), ()))
INNER_DIMS = (((1,), (1,)), ((), ()))


def swapped(value, axis, mask):
    count = lax.axis_size(axis)
    return lax.ppermute(value, axis, [(source, source ^ mask) for source in range(count)])


def passed_back(value, axis):
    count = lax.axis_size(axis)
    return lax.ppermute(value, axis, [(source, source - 1) for source in range(1, count)])


def exchanged(chunks, axis):
    return [chunks[0]] + [swapped(chunk, axis, k) for k, chunk in enumerate(chunks) if k]


def bits_of(axis):
    count = lax.axis_size(axis)
    return [1 << n for n in range(count.bit_length() - 1)]


def gathered(value, axis):
    count = lax.axis_size(axis)
    here = lax.axis_index(axis)
    bits = bits_of(axis)
    found = {0: value}
    for bit in reversed(bits):
        for offset in list(found):
            found[offset | bit] = swapped(found[offset], axis, bit)
    parts = [found[k] for k in range(count)]
    for bit in bits:
        odd = (here & bit) != 0
        parts = [jnp.where(odd, parts[k ^ bit], parts[k]) for k in range(count)]
    return jnp.concatenate(parts, axis=1)


def dispatch(routes, weights, tokens, cotangent, experts, capacity):
    tok_rows, width = tokens.shape
    slots = experts * capacity

    def kernel(here, routes, weights, tokens, cotangent, payload, places):
        rel = routes[...] ^ here[0]
        rel_a, rel_b = rel[0:1], rel[1:2]
        ids = lax.broadcasted_iota(jnp.int32, (experts, tok_rows), 0)
        hit_a, hit_b = ids == rel_a, ids == rel_b
        hits = jnp.where(hit_a | hit_b, 1.0, 0.0).astype(jnp.bfloat16)
        before = lax.broadcasted_iota(jnp.int32, (tok_rows, tok_rows), 0)
        after = lax.broadcasted_iota(jnp.int32, (tok_rows, tok_rows), 1)
        tri = jnp.where(before < after, 1.0, 0.0).astype(jnp.bfloat16)
        rank = jnp.dot(hits, tri, preferred_element_type=jnp.float32)
        rank_a = jnp.sum(jnp.where(hit_a, rank, 0.0), axis=0, keepdims=True).astype(jnp.int32)
        rank_b = jnp.sum(jnp.where(hit_b, rank, 0.0), axis=0, keepdims=True).astype(jnp.int32)
        slot = lax.broadcasted_iota(jnp.int32, (slots, tok_rows), 0)
        at_a = slot == rel_a * capacity + rank_a
        at_b = slot == rel_b * capacity + rank_b
        place = jnp.where(at_a | at_b, 1.0, 0.0).astype(jnp.bfloat16)
        scale = jnp.sum(
            jnp.where(at_a, weights[0:1], 0.0) + jnp.where(at_b, weights[1:2], 0.0),
            axis=1,
            keepdims=True,
        )
        places[...] = place
        payload[:, :width] = jnp.dot(place, tokens[...], preferred_element_type=jnp.float32).astype(
            jnp.bfloat16
        )
        picked = jnp.dot(place, cotangent[...], preferred_element_type=jnp.float32)
        payload[:, width:] = (scale * picked).astype(jnp.bfloat16)

    here = lax.axis_index("sp").astype(jnp.int32).reshape(1)
    whole = pl.BlockSpec(memory_space=pltpu.VMEM)
    return pl.pallas_call(
        kernel,
        out_shape=(
            jax.ShapeDtypeStruct((slots, 2 * width), jnp.bfloat16),
            jax.ShapeDtypeStruct((slots, tok_rows), jnp.bfloat16),
        ),
        in_specs=[pl.BlockSpec(memory_space=pltpu.SMEM)] + [whole] * 4,
        out_specs=(whole, whole),
        name="dispatch",
    )(here, routes.T, weights.T, tokens, cotangent)


def body(
    out_cotangent,
    expert_input,
    routes,
    route_weights,
    gate_proj,
    up_proj,
    down_proj,
    conv_out,
    conv_mean,
    conv_rstd,
    norm_gain,
    taps,
    out_proj,
):
    tok_rows, local_width = out_cotangent.shape
    experts = lax.axis_size("sp")
    width_parts = lax.axis_size("tp")
    full_width = local_width * width_parts
    capacity = 3 * tok_rows // experts
    sp_at = lax.axis_index("sp")
    tp_at = lax.axis_index("tp")
    payload, places = dispatch(
        routes, route_weights, expert_input, out_cotangent, experts, capacity
    )

    def chunked(value):
        return [value[k * capacity : (k + 1) * capacity] for k in range(experts)]

    arrived = exchanged(chunked(payload), "sp")
    rows_mid = jnp.concatenate([chunk[:, :local_width] for chunk in arrived], axis=0)
    cots_mid = jnp.concatenate([chunk[:, local_width:] for chunk in arrived], axis=0)
    rows_in = gathered(rows_mid, "tp")
    cot_in = gathered(cots_mid, "tp")
    gate_local = gate_proj[0]
    up_local = up_proj[0]
    down_local = down_proj[0]

    conv_ready, _ = lax.optimization_barrier((conv_out, cots_mid))
    normed = (conv_ready.astype(jnp.float32) - conv_mean[:, None]) * conv_rstd[:, None]
    scaled = normed * norm_gain[None, :]
    scaled_sigmoid = jax.nn.sigmoid(scaled)
    swished = (scaled * scaled_sigmoid).astype(jnp.bfloat16)
    swished_all = jnp.concatenate(exchanged([swished] * experts, "sp"), axis=0)

    gate_pre = jnp.dot(rows_in, gate_local, preferred_element_type=jnp.float32)
    up_pre = jnp.dot(rows_in, up_local, preferred_element_type=jnp.float32)
    gate_sigmoid = jax.nn.sigmoid(gate_pre)
    activation = (gate_pre * gate_sigmoid * up_pre).astype(jnp.bfloat16)
    act_grad = lax.dot_general(cot_in, down_local, INNER_DIMS, preferred_element_type=jnp.float32)
    gate_back = (act_grad * up_pre * gate_sigmoid * (1.0 + gate_pre * (1.0 - gate_sigmoid))).astype(
        jnp.bfloat16
    )
    up_back = (act_grad * gate_pre * gate_sigmoid).astype(jnp.bfloat16)

    down_grad = lax.dot_general(
        activation, cot_in, OUTER_DIMS, preferred_element_type=jnp.float32
    ).astype(jnp.bfloat16)[None]
    gate_grad = lax.dot_general(
        rows_in, gate_back, OUTER_DIMS, preferred_element_type=jnp.float32
    ).astype(jnp.bfloat16)[None]
    up_grad = lax.dot_general(
        rows_in, up_back, OUTER_DIMS, preferred_element_type=jnp.float32
    ).astype(jnp.bfloat16)[None]
    def partial_block(mask):
        start = (tp_at ^ mask) * local_width
        gate_rows = lax.dynamic_slice_in_dim(gate_local, start, local_width, axis=0)
        up_rows = lax.dynamic_slice_in_dim(up_local, start, local_width, axis=0)
        return lax.dot_general(
            gate_back, gate_rows, INNER_DIMS, preferred_element_type=jnp.float32
        ) + lax.dot_general(up_back, up_rows, INNER_DIMS, preferred_element_type=jnp.float32)

    covers = [down_grad, gate_grad]

    def summed_over(offsets, bit):
        if bit == 0:
            return partial_block(offsets)
        lower = bit // 2
        away = summed_over(offsets | bit, lower).astype(jnp.bfloat16)
        away = swapped(away, "tp", bit)
        if bit == width_parts // 2:
            away, covers[0], covers[1] = lax.optimization_barrier((away, covers[0], covers[1]))
        return summed_over(offsets, lower) + away.astype(jnp.float32)

    summed = summed_over(0, width_parts // 2).astype(jnp.bfloat16)
    down_grad, gate_grad = covers
    routed = jnp.concatenate(exchanged(chunked(summed), "sp"), axis=0)
    routed_sum = lax.dot_general(places, routed, OUTER_DIMS, preferred_element_type=jnp.float32)
    stream = (out_cotangent.astype(jnp.float32) + routed_sum).astype(jnp.bfloat16)
    stream_whole = gathered(stream, "tp")

    feature_rows = full_width // experts
    feature_chunks = [
        lax.dynamic_slice_in_dim(stream_whole, (sp_at ^ k) * feature_rows, feature_rows, axis=1)
        for k in range(experts)
    ]
    stream_all = jnp.concatenate(exchanged(feature_chunks, "sp"), axis=0)
    proj_grad = lax.dot_general(
        stream_all, swished_all, OUTER_DIMS, preferred_element_type=jnp.float32
    )

    swished_grad = jnp.dot(stream_whole, out_proj, preferred_element_type=jnp.float32)
    scaled_grad = (
        swished_grad * scaled_sigmoid * (1.0 + scaled * (1.0 - scaled_sigmoid)) * norm_gain[None, :]
    )
    stat_parts = jnp.stack([jnp.sum(scaled_grad, axis=1), jnp.sum(scaled_grad * normed, axis=1)])
    stat_sums = stat_parts
    for mask in range(1, width_parts):
        stat_sums = stat_sums + swapped(stat_parts, "tp", mask)
    first_mean = stat_sums[0][:, None] / full_width
    second_mean = stat_sums[1][:, None] / full_width
    conv_grad = conv_rstd[:, None] * (scaled_grad - first_mean - normed * second_mean)
    halo_rows = taps.shape[0] - 1
    following = passed_back(conv_grad[:halo_rows].astype(jnp.bfloat16), "sp").astype(jnp.float32)
    extended = jnp.concatenate([conv_grad, following], axis=0)
    conv_sum = jnp.zeros((tok_rows, local_width), jnp.float32)
    for offset in range(halo_rows + 1):
        conv_sum = conv_sum + taps[offset][None, :] * extended[offset : offset + tok_rows]
    return (gate_grad, up_grad, down_grad, proj_grad, stream, conv_sum.astype(jnp.bfloat16))


def solution(mesh):
    in_specs = (
        P("sp", "tp"),
        P("sp", "tp"),
        P("sp", None),
        P("sp", None),
        P("sp", None, "tp"),
        P("sp", None, "tp"),
        P("sp", "tp", None),
        P("sp", "tp"),
        P("sp"),
        P("sp"),
        P("tp"),
        P(None, "tp"),
        P(None, "tp"),
    )
    out_specs = (
        P("sp", None, "tp"),
        P("sp", None, "tp"),
        P("sp", "tp", None),
        P("sp", "tp"),
        P("sp", "tp"),
        P("sp", "tp"),
    )
    return jax.shard_map(body, mesh=mesh, in_specs=in_specs, out_specs=out_specs, check_vma=False)
```
